32 devices in a mesh: sp: 16 (over z, y, x), tp: 2 (over core).
Axes of the slice: x: 2, y: 2, z: 4, core: 2. Of those that a mesh axis runs over, the one named last changes fastest.
Arguments:
- latent: bfloat16 [4096, 2048], P(('sp', 'tp')), may hold values from -3 to 3
- context: bfloat16 [1024, 2048], P('sp'), may hold values from -6 to 6
- condition: float32 [2048], replicated, may hold values from -6 to 6
- ctx_cond: float32 [2048], replicated, may hold values from -6 to 6
- norm_gain: float32 [2048], replicated, may hold values from 0.1 to 1.9
- w_shift: bfloat16 [2048, 2048], P('sp', 'tp'), may hold values from -0.25 to 0.25
- w_scale: bfloat16 [2048, 2048], P('sp', 'tp'), may hold values from -0.25 to 0.25
- w_gate: bfloat16 [2048, 2048], P('sp', 'tp'), may hold values from -0.25 to 0.25
- w_query: bfloat16 [2048, 2048], P(None, 'tp'), may hold values from -0.125 to 0.125
- w_key: bfloat16 [2048, 2048], P(None, 'tp'), may hold values from -0.125 to 0.125
- w_value: bfloat16 [2048, 2048], P(None, 'tp'), may hold values from -0.125 to 0.125
- w_out: bfloat16 [2048, 2048], P('tp'), may hold values from -0.125 to 0.125
- rel_bias: float32 [16, 15, 31], replicated, may hold values from 2 to 250
Outputs:
- updated: bfloat16 [4096, 2048], P(('sp', 'tp'))
The draws below stay inside these ranges and needn't reach their ends.
All inputs are finite; a program needn't handle non-finite values.
Results may differ from the reference program's by a relative error of at most 0.015.
Values may be sent and summed in bfloat16 or wider, within the bound.
A program may use at most 128 MiB of HBM per device.

```python
import jax
import jax.numpy as jnp
import numpy as np
from jax import lax

D = 2048
HEADS = 16
HEAD_DIM = 128
GRID_W = 32
WIN_H = 8
WIN_W = 16
CTX = 1024
TOKENS = 4096
N_TP = 2


def draw_rel_bias(key, part):
    drawn = jax.random.uniform(key, (HEADS, 2 * WIN_H - 1, 2 * WIN_W - 1), jnp.float32, 2.0, 4.0)
    return drawn


def steps_of(stream_key, dims, split, low, largest):
    loudness, own = 1.0, jax.random.fold_in(stream_key, 6)
    for axis_at, blocks in split:
        steps = jnp.exp(jax.random.uniform(jax.random.fold_in(own, axis_at), (blocks,), jnp.float32, low / len(split), largest / len(split)))
        loudness = loudness * jnp.repeat(steps, dims[axis_at] // blocks).reshape([-1 if axis == axis_at else 1 for axis in range(len(dims))])
    return loudness


def noise(own_key, dims, deviation, limit, shards=(), held_as=jnp.bfloat16):
    level = steps_of(own_key, dims, shards, -0.22, 0.18) if shards else 1.0
    values = jax.random.normal(own_key, dims, jnp.float32) * deviation * level
    return jnp.minimum(jnp.maximum(values, -limit), limit).astype(held_as)


def setup_inputs(seed: int = 0) -> dict:
    splits = jax.random.split(jax.random.key(seed), 14)
    return {
        "latent": noise(splits[0], (TOKENS, D), 0.5, 3.0, ((0, 32),)),
        "context": noise(splits[1], (CTX, D), 1.0, 6.0, ((0, 16),)),
        "condition": noise(splits[2], (D,), 1.0, 6.0, (), jnp.float32),
        "ctx_cond": noise(splits[3], (D,), 1.0, 6.0, (), jnp.float32),
        "norm_gain": jnp.clip(1.0 + 0.18 * jax.random.normal(splits[4], (D,), jnp.float32), 0.1, 1.9),
        "w_shift": noise(splits[5], (D, D), (D // 4) ** -0.5, 0.25, ((0, 16), (1, 2))),
        "w_scale": noise(splits[6], (D, D), (D // 4) ** -0.5, 0.25, ((0, 16), (1, 2))),
        "w_gate": noise(splits[7], (D, D), (D // 4) ** -0.5, 0.25, ((0, 16), (1, 2))),
        "w_query": noise(splits[8], (D, D), D ** -0.5, 0.125, ((1, 2),)),
        "w_key": noise(splits[9], (D, D), D ** -0.5, 0.125, ((1, 2),)),
        "w_value": noise(splits[10], (D, D), D ** -0.5, 0.125, ((1, 2),)),
        "w_out": noise(splits[11], (D, D), D ** -0.5, 0.125, ((0, 2),)),
        "rel_bias": draw_rel_bias(jax.random.fold_in(splits[13], 71), 0),
    }


NORM_EPS = 1e-06
NEG_BIG = -1e+30

def rms_mod(block, norm_gain, shifts, scales):
    block = block.astype(jnp.float32)
    normed = block * lax.rsqrt(lax.optimization_barrier(jnp.mean(block * block, axis=-1, keepdims=True)) + NORM_EPS) * norm_gain
    return (normed * (1.0 + scales) + shifts).astype(jnp.bfloat16)

def project(block, weight):
    return jnp.dot(block, weight, preferred_element_type=jnp.float32).astype(jnp.bfloat16)

def geometry(total_rows):
    row_ids = np.arange(total_rows)
    starts = np.clip(row_ids - WIN_H // 2, 0, total_rows - WIN_H)
    row_index = starts[:, None] + np.arange(WIN_H)[None, :]
    row_off = row_index - row_ids[:, None] + WIN_H - 1
    col_ids = np.arange(GRID_W)
    col_start = np.clip(col_ids - WIN_W // 2, 0, GRID_W - WIN_W)
    col_in = (col_ids[None, :] >= col_start[:, None]) & (col_ids[None, :] < col_start[:, None] + WIN_W)
    col_off = np.clip(col_ids[None, :] - col_ids[:, None], 1 - WIN_W, WIN_W - 1) + WIN_W - 1
    return (row_index, row_off, col_in, col_off)

def reference(latent, context, condition, ctx_cond, norm_gain, w_shift, w_scale, w_gate, w_query, w_key, w_value, w_out, rel_bias):
    activated = jax.nn.silu(jnp.stack([condition, ctx_cond])).astype(jnp.bfloat16)
    shifts = jnp.dot(activated, w_shift, preferred_element_type=jnp.float32)
    scales = jnp.dot(activated, w_scale, preferred_element_type=jnp.float32)
    gate_vec = jnp.dot(activated[:1], w_gate, preferred_element_type=jnp.float32)[0]
    normed = rms_mod(latent, norm_gain, shifts[0], scales[0])
    ctx_normed = rms_mod(context, norm_gain, shifts[1], scales[1])
    queries = project(normed, w_query)
    lat_keys = project(normed, w_key)
    lat_values = project(normed, w_value)
    ctx_keys = project(ctx_normed, w_key)
    ctx_values = project(ctx_normed, w_value)
    total_rows = latent.shape[0] // GRID_W
    row_index, row_off, col_in, col_off = geometry(total_rows)
    inv_scale = HEAD_DIM ** (-0.5)

    def grid_heads(array):
        return jnp.transpose(array.reshape(total_rows, GRID_W, HEADS, HEAD_DIM), (2, 0, 1, 3))

    def ctx_heads(array):
        return jnp.transpose(array.reshape(-1, HEADS, HEAD_DIM), (1, 0, 2))

    def per_head(operands):
        query_head, key_head, value_head, ctx_key_head, ctx_value_head, bias_table = operands
        query_f = query_head.astype(jnp.float32)
        key_win = key_head[row_index].astype(jnp.float32)
        val_win = value_head[row_index].astype(jnp.float32)
        bias_win = bias_table[row_off[:, None, :, None], col_off[None, :, None, :]]
        scores_win = jnp.einsum('rqd,rkwd->rqkw', query_f, key_win) * inv_scale + bias_win
        scores_win = jnp.where(col_in[None, :, None, :], scores_win, NEG_BIG)
        scores_ctx = jnp.einsum('rqd,cd->rqc', query_f, ctx_key_head.astype(jnp.float32)) * inv_scale
        row_max = jnp.maximum(lax.optimization_barrier(jnp.max(scores_win, axis=(2, 3))), lax.optimization_barrier(jnp.max(scores_ctx, axis=2)))
        exp_win = jnp.exp(scores_win - row_max[:, :, None, None])
        exp_ctx = jnp.exp(scores_ctx - row_max[:, :, None])
        row_total = lax.optimization_barrier(jnp.sum(exp_win, axis=(2, 3))) + lax.optimization_barrier(jnp.sum(exp_ctx, axis=2))
        probs_win = (exp_win / row_total[:, :, None, None]).astype(jnp.bfloat16)
        probs_ctx = (exp_ctx / row_total[:, :, None]).astype(jnp.bfloat16)
        mixed_head = jnp.einsum('rqkw,rkwd->rqd', probs_win.astype(jnp.float32), val_win)
        mixed_head = mixed_head + jnp.einsum('rqc,cd->rqd', probs_ctx.astype(jnp.float32), ctx_value_head.astype(jnp.float32))
        return mixed_head.astype(jnp.bfloat16)
    attended = lax.map(per_head, (grid_heads(queries), grid_heads(lat_keys), grid_heads(lat_values), ctx_heads(ctx_keys), ctx_heads(ctx_values), rel_bias))
    attended = jnp.transpose(attended, (1, 2, 0, 3)).reshape(-1, HEADS * HEAD_DIM)
    head_cols = HEADS // N_TP * HEAD_DIM
    branch = jnp.zeros(latent.shape, jnp.float32)
    for group_idx in range(N_TP):
        low = group_idx * head_cols
        part_sum = jnp.dot(attended[:, low:low + head_cols], w_out[low:low + head_cols], preferred_element_type=jnp.float32).astype(jnp.bfloat16)
        part_sum = lax.optimization_barrier(part_sum)
        branch = branch + part_sum.astype(jnp.float32)
    return (latent.astype(jnp.float32) + gate_vec * branch).astype(jnp.bfloat16)
```

```python
import functools

import jax
import jax.numpy as jnp
from jax import lax
from jax.experimental import pallas as pl
from jax.experimental.pallas import tpu as pltpu
from jax.sharding import PartitionSpec as P

HEAD_DIM = 128
GRID_W = 32
WIN_H = 8
WIN_W = 16
HALF = WIN_H // 2
INNER = 4
PARTS = 4
VECS = 5
LANES = 128
NORM_EPS = 1e-06
NEG_BIG = -1e30
LOG2E = 1.4426950408889634
MESH = pl.DeviceIdType.MESH
VMEM = pltpu.VMEM


def layer_kernel(
    sp, tp, cond_ref, cctx_ref, gain_ref, tab_ref,
    wsh_hbm, wsc_hbm, wg_hbm, lat_hbm, ctx_hbm, wq_hbm, wk_hbm, wv_hbm, wo_hbm,
    out_ref,
    wsh, wsc, wg, mod_out, lat_out, ctx_out, wq, wk, wv, wo, affine, gate, nbuf0, nbuf1,
    q_buf, k_buf, v_buf, bias, att, ybuf, rbuf,
    in_sem, w_sem, x_send, x_recv,
    in_buf, out_buf, mi_send, mi_recv, mo_send, mo_recv, mf_send, mf_recv,
    own_send, own_recv, h_send, h_recv, hf_send, hf_recv,
    z_send, z_recv, n_send, n_recv, d_send, d_recv, f_send, f_recv,
):
    s = lax.axis_index("sp")
    t = lax.axis_index("tp")
    n_o = sp // INNER
    o = s // INNER
    i = lax.rem(s, INNER)
    rows, width = lat_hbm.shape
    crow = ctx_hbm.shape[0]
    cw = width // tp
    hw = max(LANES, 3 * cw // 4 // LANES * LANES)
    tokens = rows * tp
    halo = tokens // 2
    n_lat = 2 * tokens
    cols = wq.shape[1]
    heads = cols // HEAD_DIM
    mod_cols = wsh.shape[1]
    n_piece = mod_cols // LANES

    def remote(src, dst, ss, rs, dev):
        return pltpu.make_async_remote_copy(
            src_ref=src, dst_ref=dst, send_sem=ss, recv_sem=rs,
            device_id=dev, device_id_type=MESH,
        )

    def at(oo, ii):
        return (oo * INNER + ii, t)

    def held(j):
        if j == 0:
            return o
        low, high = o, n_o - 1 - o
        both = jnp.minimum(low, high)
        step = (j + 1) // 2
        near = o - step if j % 2 else o + step
        far = jnp.where(low < high, o + (j - both), o - (j - both))
        return jnp.where(j <= 2 * both, near, far)

    def outer(d):
        return lax.rem(o + d, n_o)

    def inner(d):
        return lax.rem(i + d, INNER)

    def tp_peer(d):
        return lax.rem(t + d, tp)

    ix = i + 1 - 2 * lax.rem(i, 2)
    iy = lax.rem(i + 2, INNER)
    ixy = lax.rem(ix + 2, INNER)
    nbr = (ix, iy)
    nxt = lax.rem(s + 1, sp)
    prv = lax.rem(s + sp - 1, sp)

    barrier = pltpu.get_barrier_semaphore()

    def greet(dev):
        pl.semaphore_signal(barrier, inc=1, device_id=dev, device_id_type=MESH)

    for d in range(1, n_o):
        greet(at(outer(d), i))
    for d in range(1, INNER):
        greet(at(o, inner(d)))
    for d in range(1, tp):
        greet((s, tp_peer(d)))
    greet((nxt, t))
    greet((prv, t))

    def own_rows(who):
        return lat_out.at[pl.ds(pl.multiple_of(halo + who * rows, rows), rows), :]

    first = [
        pltpu.make_async_copy(src, dst, in_sem.at[n])
        for n, (src, dst) in enumerate(
            (
                (wsh_hbm, wsh), (wsc_hbm, wsc), (wg_hbm, wg),
                (ctx_hbm, ctx_out.at[pl.ds(pl.multiple_of(s * crow, crow), crow), :]),
                (lat_hbm, own_rows(t)),
            )
        )
    ]
    loads = [
        pltpu.make_async_copy(src, dst, w_sem.at[n])
        for n, (src, dst) in enumerate(
            ((wq_hbm, wq), (wk_hbm, wk), (wv_hbm, wv), (wo_hbm, wo))
        )
    ]
    for copy in first:
        copy.start()

    row_part = wsh.shape[0]
    begin = s * row_part

    def act_of(ref):
        if row_part % LANES == 0:
            x = ref[:, pl.ds(pl.multiple_of(begin, LANES), row_part)]
            x = jnp.broadcast_to(x, (8, row_part))
        else:
            base = begin // LANES * LANES
            x = jnp.broadcast_to(ref[:, pl.ds(pl.multiple_of(base, LANES), LANES)], (8, LANES))
            x = pltpu.roll(x, lax.rem(LANES - (begin - base), LANES), 1)[:, :row_part]
        return x * jax.nn.sigmoid(x)

    act_a, act_c = act_of(cond_ref), act_of(cctx_ref)
    sub = lax.broadcasted_iota(jnp.int32, (8, row_part), 0)

    def act(k):
        both = jnp.where(sub == 2 * k, act_a, 0.0)
        if k < 2:
            both = jnp.where(sub == 2 * k + 1, act_c, both)
        return both.astype(jnp.bfloat16)

    for copy in first[:3]:
        copy.wait()
    val = (
        jnp.dot(act(0), wsh[...], preferred_element_type=jnp.float32)
        + jnp.dot(act(1), wsc[...], preferred_element_type=jnp.float32)
        + jnp.dot(act(2), wg[...], preferred_element_type=jnp.float32)
    )
    for c in range(n_piece):
        in_buf[pl.ds(i, 1), VECS * c : VECS * (c + 1), :] = val[
            :VECS, c * LANES : (c + 1) * LANES
        ][None]

    pl.semaphore_wait(barrier, n_o - 1 + INNER - 1 + tp - 1 + 2)

    def mod_in(d, who):
        return remote(
            in_buf.at[who], in_buf.at[who], mi_send.at[d], mi_recv.at[d], at(o, inner(d))
        )

    def mod_across(d, who):
        return remote(
            out_buf.at[who], out_buf.at[who], mo_send.at[d], mo_recv.at[d], at(outer(d), i)
        )

    def mod_fwd(d, who):
        return remote(
            mod_out.at[who], mod_out.at[who], mf_send.at[d], mf_recv.at[d], (s, tp_peer(d))
        )

    for d in range(1, INNER):
        mod_in(d, i).start()

    def own_copy(d, who):
        return remote(
            own_rows(who), own_rows(who), own_send.at[d], own_recv.at[d], (s, tp_peer(d))
        )

    halos = []
    for who in range(tp):
        down = who >= tp // 2
        for p in range(rows // GRID_W):
            low = who * rows + p * GRID_W
            if down:
                off = low - halo
            elif low < (HALF - 1) * GRID_W:
                off = halo + tokens + low
            else:
                continue
            halos.append(
                (
                    p, who, halo + low, off, (nxt, t) if down else (prv, t),
                    (s < sp - 1) if down else (s > 0), (s > 0) if down else (s < sp - 1),
                )
            )

    def halo_copy(p, low, off, dev):
        return remote(
            lat_out.at[pl.ds(low, GRID_W), :], lat_out.at[pl.ds(off, GRID_W), :],
            h_send.at[p], h_recv.at[p], dev,
        )

    def halo_fwd(p, who, off, e):
        ref = lat_out.at[pl.ds(off, GRID_W), :]
        return remote(ref, ref, hf_send.at[e, p], hf_recv.at[who, p], (s, tp_peer(e)))

    def halo_start(piece):
        for p, who, low, off, dev, gives, takes in halos:
            if p == piece:
                @pl.when((t == who) & gives)
                def _():
                    halo_copy(p, low, off, dev).start()

    def halo_relay():
        for p, who, low, off, dev, gives, takes in halos:
            @pl.when((t == who) & takes)
            def _():
                halo_copy(p, low, off, dev).wait_recv()
                for e in range(1, tp):
                    halo_fwd(p, who, off, e).start()

    def halo_in():
        for p, who, low, off, dev, gives, takes in halos:
            @pl.when((t != who) & takes)
            def _():
                halo_fwd(p, who, off, 1).wait_recv()

    def halo_drain():
        for p, who, low, off, dev, gives, takes in halos:
            @pl.when((t == who) & gives)
            def _():
                halo_copy(p, low, off, dev).wait_send()

            @pl.when((t == who) & takes)
            def _():
                for e in range(1, tp):
                    halo_fwd(p, who, off, e).wait_send()

    def block(oo, ii, who, half=None):
        low, size = ((0, cw), (0, hw), (hw, cw - hw))[0 if half is None else half + 1]
        return ctx_out.at[
            pl.ds(pl.multiple_of((oo * INNER + ii) * crow, crow), crow),
            pl.ds(pl.multiple_of(who * cw + low, LANES), size),
        ]

    def line(src, way):
        ref = block(src, i, t)
        to = jnp.clip(o + 2 * way - 1, 0, n_o - 1)
        return remote(ref, ref, z_send.at[src, way], z_recv.at[src], at(to, i))

    def onward(src, way):
        return (src <= o) & (o < n_o - 1) if way else (src >= o) & (o > 0)

    def line_send(src):
        for way in range(2):
            @pl.when(onward(src, way))
            def _():
                line(src, way).start()

    def line_drain(src):
        for way in range(2):
            @pl.when(onward(src, way))
            def _():
                line(src, way).wait_send()

    def side(j, a, ii):
        ref = block(held(j), ii, t)
        return remote(ref, ref, n_send.at[j, a], n_recv.at[j, a], at(o, nbr[a]))

    def diag(j, a, ii):
        ref = block(held(j), ii, t, a)
        return remote(ref, ref, d_send.at[j, a], d_recv.at[j, a], at(o, nbr[1 - a]))

    def share(e, j, k, who):
        half = None if k < 3 else k - 3
        ref = block(held(j), (i, ix, iy, ixy, ixy)[k], who, half)
        return remote(
            ref, ref, f_send.at[e, j, k], f_recv.at[e, j, k], (s, tp_peer(e))
        )

    def share_all(j, k):
        for e in range(1, tp):
            share(e, j, k, t).start()

    def lines_in(j):
        line(held(j), 0).wait_recv()
        line_send(held(j))
        for a in range(2):
            side(j, a, i).start()
        share_all(j, 0)

    def relay(j):
        for a in range(2):
            side(j, a, nbr[a]).wait_recv()
            diag(j, a, nbr[a]).start()
            share_all(j, 1 + a)

    def relay_diag(j):
        for a in range(2):
            diag(j, a, ixy).wait_recv()
            share_all(j, 3 + a)

    def shares_in(j):
        for k in range(5):
            if j == 0 and k == 0:
                continue
            for e in range(1, tp):
                share(e, j, k, lax.rem(t + tp - e, tp)).wait_recv()

    first[3].wait()
    first[4].wait()
    for load in loads:
        load.start()
    for a in range(2):
        side(0, a, i).start()
    line_send(o)
    for d in range(1, tp):
        own_copy(d, t).start()

    lat_out[n_lat - GRID_W :, :] = jnp.zeros((GRID_W, width), jnp.bfloat16)

    @pl.when(s == 0)
    def _():
        lat_out[:halo, :] = jnp.zeros((halo, width), jnp.bfloat16)

    @pl.when(s == sp - 1)
    def _():
        lat_out[halo + tokens : n_lat - GRID_W, :] = jnp.zeros(
            (halo - GRID_W, width), jnp.bfloat16
        )

    def build_bias(low, high):
        grid_rows = tokens // GRID_W
        lanes = lax.broadcasted_iota(jnp.int32, (GRID_W, 128), 1)
        cq = lax.broadcasted_iota(jnp.int32, (GRID_W, 128), 0)
        c2 = lax.rem(lanes, GRID_W)
        group = lanes // GRID_W
        cs = jnp.clip(cq - WIN_W // 2, 0, GRID_W - WIN_W)
        col_in = (c2 >= cs) & (c2 < cs + WIN_W)
        per = 128 // GRID_W
        start = s * grid_rows
        kr = lax.broadcasted_iota(jnp.int32, (GRID_W, n_lat), 1) // GRID_W

        def body(h, c):
            v_buf[:, pl.ds(pl.multiple_of(h * 2 * HEAD_DIM + HEAD_DIM, HEAD_DIM), HEAD_DIM)] = (
                jnp.ones((v_buf.shape[0], HEAD_DIM), jnp.bfloat16)
            )
            groups = []
            for k in range(24 // per):
                part = jnp.full((GRID_W, 128), NEG_BIG, jnp.float32)
                for g in range(per):
                    if not HALF <= per * k + g < HALF + tab_ref.shape[1]:
                        continue
                    at_row = per * k + g - HALF
                    row = tab_ref[h, at_row : at_row + 1, :] * LOG2E
                    rolled = pltpu.roll(
                        jnp.broadcast_to(row, (GRID_W, 128)),
                        (GRID_W * g - (WIN_W - 1)) % 128, 1, stride=1, stride_axis=0,
                    )
                    part = jnp.where(group == g, rolled, part)
                groups.append(jnp.where(col_in, part, NEG_BIG))
            table = jnp.concatenate(groups, axis=1)
            total = table.shape[1]
            for r in range(grid_rows):
                shift = (grid_rows - 1 - r) * GRID_W
                strip = table if shift == 0 else pltpu.roll(table, total - shift, 1)
                lo = jnp.clip(start + r - HALF, 0, grid_rows * sp - WIN_H) - start + HALF
                bias[h, r * GRID_W : (r + 1) * GRID_W, :] = jnp.where(
                    (kr >= lo) & (kr < lo + WIN_H), strip[:, :n_lat], NEG_BIG
                )
            return c

        lax.fori_loop(low, high, body, 0, unroll=min(2, high - low))

    build_bias(0, heads // 2)
    halo_start(0)
    for d in range(1, INNER):
        mod_in(d, i).wait_send()
    for d in range(1, INNER):
        mod_in(d, lax.rem(i + INNER - d, INNER)).wait_recv()
    out_buf[pl.ds(o, 1)] = jnp.sum(in_buf[...], axis=0, keepdims=True)
    for d in range(1, n_o):
        mod_across(d, o).start()
    build_bias(heads // 2, heads)
    relay(0)
    lines_in(1)
    halo_start(1)

    for d in range(1, n_o):
        mod_across(d, o).wait_send()
    for d in range(1, n_o):
        mod_across(d, lax.rem(o + n_o - d, n_o)).wait_recv()
    mod_out[pl.ds(t, 1)] = jnp.sum(out_buf[...], axis=0, keepdims=True)
    for d in range(1, tp):
        mod_fwd(d, t).start()
    for d in range(1, tp):
        own_copy(d, lax.rem(t + tp - d, tp)).wait_recv()
    for d in range(1, tp):
        mod_fwd(d, lax.rem(t + tp - d, tp)).wait_recv()
    for w in range(tp):
        for c in range(n_piece):
            low = w * mod_cols + c * LANES
            cut = slice(low, low + LANES)
            for kind in range(2):
                r = VECS * c + kind
                affine[2 * kind : 2 * kind + 1, cut] = gain_ref[:, cut] * (
                    1.0 + mod_out[w, r + 2 : r + 3, :]
                )
                affine[2 * kind + 1 : 2 * kind + 2, cut] = mod_out[w, r : r + 1, :]
            gate[:, cut] = mod_out[w, VECS * c + 4 : VECS * c + 5, :]

    def norm_piece(src, src_row, dst, dst_row, count, kind):
        x = src[pl.ds(src_row, count), :].astype(jnp.float32)
        r = lax.rsqrt(jnp.mean(x * x, axis=1, keepdims=True) + NORM_EPS)
        y = x * r * affine[2 * kind : 2 * kind + 1, :] + affine[2 * kind + 1 : 2 * kind + 2, :]
        dst[dst_row : dst_row + count, :] = y.astype(jnp.bfloat16)

    STEP = 16

    def normalise(pieces, dst, kind):
        todo = []
        low = 0
        for src, row, size in pieces:
            for k in range(0, size, STEP):
                at_row = row + k
                if not isinstance(at_row, int):
                    at_row = pl.multiple_of(at_row, STEP)
                todo.append(
                    functools.partial(norm_piece, src, at_row, dst, low + k, STEP, kind)
                )
            low += size
        return todo

    def project(src, w, dst, pieces, scale=None, spread=1):
        count = sum(p[1] for p in pieces)
        cc = 2 * HEAD_DIM

        def one(n):
            y = jnp.dot(
                src[:count, :], w[:, n * cc : (n + 1) * cc], preferred_element_type=jnp.float32
            )
            if scale is not None:
                y = y * scale
            y = y.astype(jnp.bfloat16)
            low = 0
            for start, size in pieces:
                if spread == 1:
                    dst[start : start + size, n * cc : (n + 1) * cc] = y[low : low + size]
                else:
                    for k in range(2):
                        col = (2 * n + k) * cc
                        dst[start : start + size, col : col + HEAD_DIM] = y[
                            low : low + size, k * HEAD_DIM : (k + 1) * HEAD_DIM
                        ]
                low += size

        return [functools.partial(one, n) for n in range(cols // cc)]

    def run(dots, norms=()):
        done = 0
        for n, dot in enumerate(dots):
            dot()
            upto = (n + 1) * len(norms) // len(dots)
            for norm in norms[done:upto]:
                norm()
            done = upto
        for norm in norms[done:]:
            norm()

    group = n_o // PARTS
    g_rows = INNER * crow
    part_rows = group * g_rows
    own = ((halo, tokens),)
    ends = ((0, halo), (halo + tokens, halo))

    def js(c):
        return range(c * group, (c + 1) * group)

    def norm_ctx(c, dst):
        return normalise([(ctx_out, held(j) * g_rows, g_rows) for j in js(c)], dst, 1)

    def kv(src, pieces):
        return project(src, wk, k_buf, pieces) + project(src, wv, v_buf, pieces, spread=2)

    def ctx_at(c):
        return ((n_lat + c * part_rows, part_rows),)

    def each(step, c):
        for j in js(c):
            step(j)

    def line_part(c):
        for j in js(c):
            if j > 1:
                lines_in(j)

    def relay_part(c):
        for j in js(c):
            if j > 0:
                relay(j)

    halo_norm = normalise([(lat_out, 0, halo), (lat_out, halo + tokens, halo)], nbuf0, 0)

    line_part(0)
    relay_part(0)
    run([], normalise([(lat_out, halo, tokens)], nbuf0, 0))
    loads[0].wait()
    run(project(nbuf0, wq, q_buf, ((0, tokens),), HEAD_DIM ** -0.5 * LOG2E))
    relay_part(1)
    each(relay_diag, 0)
    line_part(2)
    halo_start(2)
    loads[1].wait()
    run(project(nbuf0, wk, k_buf, own))
    each(shares_in, 0)
    loads[2].wait()
    run(project(nbuf0, wv, v_buf, own, spread=2), norm_ctx(0, nbuf1))
    line_part(3)
    for p in range(3, rows // GRID_W):
        halo_start(p)
    each(relay_diag, 1)
    run(project(nbuf1, wk, k_buf, ctx_at(0)))
    relay_part(2)
    each(shares_in, 1)
    run(project(nbuf1, wv, v_buf, ctx_at(0), spread=2), norm_ctx(1, nbuf0))
    relay_part(3)
    run(project(nbuf0, wk, k_buf, ctx_at(1)))
    each(relay_diag, 2)
    halo_relay()
    run(project(nbuf0, wv, v_buf, ctx_at(1), spread=2))
    each(shares_in, 2)
    run([], norm_ctx(2, nbuf1))
    run(project(nbuf1, wk, k_buf, ctx_at(2)))
    each(relay_diag, 3)
    halo_in()
    run(project(nbuf1, wv, v_buf, ctx_at(2), spread=2), halo_norm)
    each(shares_in, 3)
    run(kv(nbuf0, ends), norm_ctx(3, nbuf1))
    run(kv(nbuf1, ctx_at(3)))

    n_all = k_buf.shape[0]

    def attend(h, c):
        cut = pl.ds(pl.multiple_of(h * HEAD_DIM, HEAD_DIM), HEAD_DIM)

        def scores(start, count):
            return lax.dot_general(
                q_buf[:, cut], k_buf[pl.ds(start, count), cut],
                (((1,), (1,)), ((), ())), preferred_element_type=jnp.float32,
            )

        win = scores(0, n_lat) + bias[h]
        ctx = scores(n_lat, n_all - n_lat)
        m = jnp.maximum(jnp.max(win, axis=1, keepdims=True), jnp.max(ctx, axis=1, keepdims=True))
        e = jnp.concatenate(
            [jnp.exp2(win - m).astype(jnp.bfloat16), jnp.exp2(ctx - m).astype(jnp.bfloat16)],
            axis=1,
        )
        y = jnp.dot(
            e, v_buf[:, pl.ds(pl.multiple_of(h * 2 * HEAD_DIM, 2 * HEAD_DIM), 2 * HEAD_DIM)],
            preferred_element_type=jnp.float32,
        )
        att[:, cut] = (y[:, :HEAD_DIM] / y[:, HEAD_DIM:]).astype(jnp.bfloat16)
        return c

    lax.fori_loop(0, heads, attend, 0, unroll=heads)

    loads[3].wait()
    n_chunk = ybuf.shape[0]
    ow = ybuf.shape[2]

    def part(c, who):
        return ybuf.at[c, pl.ds(pl.multiple_of(who * rows, rows), rows), :]

    def swap(d, c):
        return remote(
            part(c, tp_peer(d)), rbuf.at[d, c], x_send.at[d, c], x_recv.at[d, c],
            (s, tp_peer(d)),
        )

    for c in range(n_chunk):
        ybuf[c] = jnp.dot(
            att[...], wo[:, c * ow : (c + 1) * ow], preferred_element_type=jnp.float32
        ).astype(jnp.bfloat16)
        for d in range(1, tp):
            swap(d, c).start()
    for c in range(n_chunk):
        branch = part(c, t)[...].astype(jnp.float32)
        for d in range(1, tp):
            swap(d, c).wait_recv()
            branch = branch + rbuf[d, c].astype(jnp.float32)
        sl = slice(c * ow, (c + 1) * ow)
        mine = lat_out[pl.ds(pl.multiple_of(halo + t * rows, rows), rows), sl]
        out_ref[:, sl] = (mine.astype(jnp.float32) + gate[:, sl] * branch).astype(jnp.bfloat16)

    for d in range(1, tp):
        own_copy(d, t).wait_send()
        mod_fwd(d, t).wait_send()
        for c in range(n_chunk):
            swap(d, c).wait_send()
    halo_drain()
    for j in range(n_o):
        for k in range(5):
            if j == 0 and k == 0:
                continue
            for e in range(1, tp):
                share(e, j, k, t).wait_send()
        for a in range(2):
            side(j, a, i).wait_send()
            diag(j, a, nbr[a]).wait_send()
    for j in range(n_o):
        line_drain(held(j))


def layer(sp, tp, vmem, cond, cctx, gain, table, *big):
    w_shift, latent, context, w_query = big[0], big[3], big[4], big[5]
    rows, width = latent.shape
    row_part, mod_cols = w_shift.shape
    cols = w_query.shape[1]
    heads = cols // HEAD_DIM
    tokens = rows * tp
    n_lat = 2 * tokens
    n_ctx = context.shape[0] * sp
    n_o = sp // INNER
    n_chunk = max(4, tp)
    pack = -(-VECS * (mod_cols // LANES) // 8) * 8
    dma = pltpu.SemaphoreType.DMA
    spec = pl.BlockSpec(memory_space=VMEM)
    bf, f32 = jnp.bfloat16, jnp.float32
    pieces = rows // GRID_W
    step_rows = max(tokens, n_ctx // PARTS)
    return pl.pallas_call(
        functools.partial(layer_kernel, sp, tp),
        out_shape=jax.ShapeDtypeStruct(latent.shape, bf),
        in_specs=[spec] * 4 + [pl.BlockSpec(memory_space=pl.ANY)] * 9,
        out_specs=spec,
        scratch_shapes=[
            VMEM((row_part, mod_cols), bf), VMEM((row_part, mod_cols), bf),
            VMEM((row_part, mod_cols), bf),
            VMEM((tp, pack, LANES), f32),
            VMEM((n_lat, width), bf),
            VMEM((n_ctx, width), bf),
            VMEM((width, cols), bf), VMEM((width, cols), bf), VMEM((width, cols), bf),
            VMEM((cols, width), bf),
            VMEM((8, width), f32), VMEM((1, width), f32),
            VMEM((step_rows, width), bf), VMEM((step_rows, width), bf),
            VMEM((tokens, cols), bf),
            VMEM((n_lat + n_ctx, cols), bf), VMEM((n_lat + n_ctx, 2 * cols), bf),
            VMEM((heads, tokens, n_lat), f32),
            VMEM((tokens, cols), bf),
            VMEM((n_chunk, tokens, width // n_chunk), bf),
            VMEM((tp, n_chunk, rows, width // n_chunk), bf),
            dma((5,)), dma((4,)), dma((tp, n_chunk)), dma((tp, n_chunk)),
            VMEM((INNER, pack, LANES), f32),
            VMEM((n_o, pack, LANES), f32),
            dma((INNER,)), dma((INNER,)), dma((n_o,)), dma((n_o,)), dma((tp,)), dma((tp,)),
            dma((tp,)), dma((tp,)), dma((pieces,)), dma((pieces,)),
            dma((tp, pieces)), dma((tp, pieces)),
            dma((n_o, 2)), dma((n_o,)), dma((n_o, 2)), dma((n_o, 2)),
            dma((n_o, 2)), dma((n_o, 2)), dma((tp, n_o, 5)), dma((tp, n_o, 5)),
        ],
        compiler_params=pltpu.CompilerParams(
            collective_id=0, has_side_effects=True, vmem_limit_bytes=vmem
        ),
        name="layer",
    )(cond, cctx, gain, table, *big)


def on_device(
    latent, context, condition, ctx_cond, norm_gain, w_shift, w_scale, w_gate,
    w_query, w_key, w_value, w_out, rel_bias,
):
    tp = lax.axis_size("tp")
    sp = lax.axis_size("sp")
    head_dev = w_query.shape[1] // HEAD_DIM
    tokens = latent.shape[0] * tp
    halo = HALF * GRID_W
    assert tokens == 2 * halo and tp % 2 == 0 and sp % (PARTS * INNER) == 0
    table = lax.dynamic_slice_in_dim(rel_bias, lax.axis_index("tp") * head_dev, head_dev, 0)
    table = jnp.pad(table, ((0, 0), (0, 0), (0, LANES - table.shape[2])))
    return layer(
        sp, tp, 60 * 1024 * 1024, condition[None], ctx_cond[None], norm_gain[None], table,
        w_shift, w_scale, w_gate, latent, context, w_query, w_key, w_value, w_out,
    )


def solution(mesh):
    placed = (
        P(("sp", "tp"), None),
        P("sp", None),
        P(),
        P(),
        P(),
        P("sp", "tp"),
        P("sp", "tp"),
        P("sp", "tp"),
        P(None, "tp"),
        P(None, "tp"),
        P(None, "tp"),
        P("tp", None),
        P(),
    )
    return jax.shard_map(
        on_device, mesh=mesh, in_specs=placed, out_specs=P(("sp", "tp"), None), check_vma=False
    )
```

```python
import functools

import jax
import jax.numpy as jnp
from jax import lax
from jax.experimental import pallas as pl
from jax.experimental.pallas import tpu as pltpu
from jax.sharding import PartitionSpec as P

HEAD_DIM = 128
GRID_W = 32
WIN_H = 8
WIN_W = 16
HALF = WIN_H // 2
INNER = 4
VECS = 5
LANES = 128
NORM_EPS = 1e-06
NEG_BIG = -1e30
LOG2E = 1.4426950408889634
MESH = pl.DeviceIdType.MESH
VMEM = pltpu.VMEM


def layer_kernel(
    sp, tp, cond_hbm, cctx_hbm, gain_hbm, tab_hbm,
    wsh_hbm, wsc_hbm, wg_hbm, lat_hbm, ctx_hbm, wq_hbm, wk_hbm, wv_hbm, wo_hbm,
    out_hbm,
    cond_ref, cctx_ref, gain_ref, tab_ref, out_ref, out_sem, wsh, wsc, wg, mod_out, lat_out, ctx_out, wq, wk, wv, wo, affine, gate, nbuf0, nbuf1,
    q_buf, k_buf, v_buf, bias, att, ybuf, rbuf,
    in_sem, w_sem, x_send, x_recv,
    in_buf, out_buf, mi_send, mi_recv, mo_send, mo_recv, mf_send, mf_recv,
    own_send, own_recv, h_send, h_recv, hf_send, hf_recv,
    z_send, z_recv, c_send, c_recv, n_send, n_recv, d_send, d_recv, f_send, f_recv,
):
    s = lax.axis_index("sp")
    t = lax.axis_index("tp")
    n_o = sp // INNER
    o = s // INNER
    i = lax.rem(s, INNER)
    rows, width = lat_hbm.shape
    crow = ctx_hbm.shape[0]
    cw = width // tp
    hw = max(LANES, 3 * cw // 4 // LANES * LANES)
    tokens = rows * tp
    halo = tokens // 2
    n_lat = 2 * tokens
    cols = wq.shape[1]
    heads = cols // HEAD_DIM
    mod_cols = wsh.shape[1]
    n_piece = mod_cols // LANES

    def remote(src, dst, ss, rs, dev):
        return pltpu.make_async_remote_copy(
            src_ref=src, dst_ref=dst, send_sem=ss, recv_sem=rs,
            device_id=dev, device_id_type=MESH,
        )

    def at(oo, ii):
        return (oo * INNER + ii, t)

    def held(j):
        if j == 0:
            return o
        low, high = o, n_o - 1 - o
        both = jnp.minimum(low, high)
        step = (j + 1) // 2
        near = o - step if j % 2 else o + step
        far = jnp.where(low < high, o + (j - both), o - (j - both))
        return jnp.where(j <= 2 * both, near, far)

    def outer(d):
        return lax.rem(o + d, n_o)

    def inner(d):
        return lax.rem(i + d, INNER)

    def tp_peer(d):
        return lax.rem(t + d, tp)

    ix = i + 1 - 2 * lax.rem(i, 2)
    iy = lax.rem(i + 2, INNER)
    ixy = lax.rem(ix + 2, INNER)
    nbr = (ix, iy)
    nxt = lax.rem(s + 1, sp)
    prv = lax.rem(s + sp - 1, sp)

    barrier = pltpu.get_barrier_semaphore()

    def greet(dev):
        pl.semaphore_signal(barrier, inc=1, device_id=dev, device_id_type=MESH)

    for d in range(1, n_o):
        greet(at(outer(d), i))
    for d in range(1, INNER):
        greet(at(o, inner(d)))
    for d in range(1, tp):
        greet((s, tp_peer(d)))
    for way, to in ((s < sp - 1, nxt), (s > 0, prv)):
        @pl.when(way)
        def _():
            greet((to, t))

    def own_rows(who):
        return lat_out.at[pl.ds(pl.multiple_of(halo + who * rows, rows), rows), :]

    first = [
        pltpu.make_async_copy(src, dst, in_sem.at[n])
        for n, (src, dst) in enumerate(
            (
                (cond_hbm, cond_ref), (cctx_hbm, cctx_ref),
                (wsh_hbm, wsh), (wsc_hbm, wsc), (wg_hbm, wg),
                (gain_hbm, gain_ref), (tab_hbm, tab_ref),
                (ctx_hbm, ctx_out.at[pl.ds(pl.multiple_of(s * crow, crow), crow), :]),
                (lat_hbm, own_rows(t)),
            )
        )
    ]
    loads = [
        pltpu.make_async_copy(src, dst, w_sem.at[n])
        for n, (src, dst) in enumerate(
            ((wq_hbm, wq), (wk_hbm, wk), (wv_hbm, wv), (wo_hbm, wo))
        )
    ]
    for copy in first:
        copy.start()

    row_part = wsh.shape[0]
    begin = s * row_part

    def act_of(ref):
        if row_part % LANES == 0:
            x = ref[:, pl.ds(pl.multiple_of(begin, LANES), row_part)]
            x = jnp.broadcast_to(x, (8, row_part))
        else:
            base = begin // LANES * LANES
            x = jnp.broadcast_to(ref[:, pl.ds(pl.multiple_of(base, LANES), LANES)], (8, LANES))
            x = pltpu.roll(x, lax.rem(LANES - (begin - base), LANES), 1)[:, :row_part]
        return x * jax.nn.sigmoid(x)

    for copy in first[:5]:
        copy.wait()
    act_a, act_c = act_of(cond_ref), act_of(cctx_ref)
    sub = lax.broadcasted_iota(jnp.int32, (8, row_part), 0)

    def act(k):
        both = jnp.where(sub == 2 * k, act_a, 0.0)
        if k < 2:
            both = jnp.where(sub == 2 * k + 1, act_c, both)
        return both.astype(jnp.bfloat16)

    val = (
        jnp.dot(act(0), wsh[...], preferred_element_type=jnp.float32)
        + jnp.dot(act(1), wsc[...], preferred_element_type=jnp.float32)
        + jnp.dot(act(2), wg[...], preferred_element_type=jnp.float32)
    )
    for c in range(n_piece):
        in_buf[pl.ds(i, 1), VECS * c : VECS * (c + 1), :] = val[
            :VECS, c * LANES : (c + 1) * LANES
        ][None]

    ends_met = jnp.where(s == 0, 1, 0) + jnp.where(s == sp - 1, 1, 0)
    pl.semaphore_wait(barrier, n_o - 1 + INNER - 1 + tp - 1 + 2 - ends_met)

    def mod_in(d, who):
        return remote(
            in_buf.at[who], in_buf.at[who], mi_send.at[d], mi_recv.at[d], at(o, inner(d))
        )

    def mod_across(d, who):
        return remote(
            out_buf.at[who], out_buf.at[who], mo_send.at[d], mo_recv.at[d], at(outer(d), i)
        )

    def mod_fwd(d, who):
        return remote(
            mod_out.at[who], mod_out.at[who], mf_send.at[d], mf_recv.at[d], (s, tp_peer(d))
        )

    for d in range(1, INNER):
        mod_in(d, i).start()

    def own_copy(d, who):
        return remote(
            own_rows(who), own_rows(who), own_send.at[d], own_recv.at[d], (s, tp_peer(d))
        )

    halos = []
    for who in range(tp):
        down = who >= tp // 2
        for p in range(rows // GRID_W):
            low = who * rows + p * GRID_W
            if down:
                off = low - halo
            elif low < (HALF - 1) * GRID_W:
                off = halo + tokens + low
            else:
                continue
            halos.append(
                (
                    p, who, halo + low, off, (nxt, t) if down else (prv, t),
                    (s < sp - 1) if down else (s > 0), (s > 0) if down else (s < sp - 1),
                )
            )

    def halo_copy(p, low, off, dev):
        return remote(
            lat_out.at[pl.ds(low, GRID_W), :], lat_out.at[pl.ds(off, GRID_W), :],
            h_send.at[p], h_recv.at[p], dev,
        )

    def halo_fwd(p, who, off, e):
        ref = lat_out.at[pl.ds(off, GRID_W), :]
        return remote(ref, ref, hf_send.at[e, p], hf_recv.at[who, p], (s, tp_peer(e)))

    def halo_start(piece):
        for p, who, low, off, dev, gives, takes in halos:
            if p == piece:
                @pl.when((t == who) & gives)
                def _():
                    halo_copy(p, low, off, dev).start()

    def halo_relay():
        for p, who, low, off, dev, gives, takes in halos:
            @pl.when((t == who) & takes)
            def _():
                halo_copy(p, low, off, dev).wait_recv()
                for e in range(1, tp):
                    halo_fwd(p, who, off, e).start()

    def halo_in():
        for p, who, low, off, dev, gives, takes in halos:
            @pl.when((t != who) & takes)
            def _():
                halo_fwd(p, who, off, 1).wait_recv()

    def halo_drain():
        for p, who, low, off, dev, gives, takes in halos:
            @pl.when((t == who) & gives)
            def _():
                halo_copy(p, low, off, dev).wait_send()

            @pl.when((t == who) & takes)
            def _():
                for e in range(1, tp):
                    halo_fwd(p, who, off, e).wait_send()

    def block(oo, ii, who, half=None):
        low, size = ((0, cw), (0, hw), (hw, cw - hw))[0 if half is None else half + 1]
        return ctx_out.at[
            pl.ds(pl.multiple_of((oo * INNER + ii) * crow, crow), crow),
            pl.ds(pl.multiple_of(who * cw + low, LANES), size),
        ]

    def line(src, way):
        ref = block(src, i, t)
        to = jnp.clip(o + 2 * way - 1, 0, n_o - 1)
        return remote(ref, ref, z_send.at[src, way], z_recv.at[src], at(to, i))

    def onward(src, way):
        return (src <= o) & (o < n_o - 1) if way else (src >= o) & (o > 0)

    def line_send(src):
        for way in range(2):
            @pl.when(onward(src, way))
            def _():
                line(src, way).start()

    def cross(j, src):
        ref = block(src, ixy, t)
        return remote(ref, ref, c_send.at[j], c_recv.at[src], at(held(j), i))

    def line_drain(src):
        for way in range(2):
            @pl.when(onward(src, way))
            def _():
                line(src, way).wait_send()

    def side(j, a, ii):
        ref = block(held(j), ii, t)
        return remote(ref, ref, n_send.at[j, a], n_recv.at[j, a], at(o, nbr[a]))

    def diag(j, a, ii):
        ref = block(held(j), ii, t, a)
        return remote(ref, ref, d_send.at[j, a], d_recv.at[j, a], at(o, nbr[1 - a]))

    def share(e, j, k, who):
        half = None if k < 3 or j > 0 else k - 3
        ref = block(held(j), (i, ix, iy, ixy, ixy)[k], who, half)
        return remote(
            ref, ref, f_send.at[e, j, k], f_recv.at[e, j, k], (s, tp_peer(e))
        )

    def share_all(j, k):
        for e in range(1, tp):
            share(e, j, k, t).start()

    def lines_in(j):
        line(held(j), 0).wait_recv()
        line_send(held(j))
        for a in range(2):
            side(j, a, i).start()
        share_all(j, 0)

    outer_plane = (o == 0) | (o == n_o - 1)

    def lines_wave(far, when=True):
        for w in far:
            for j in range(1, n_o):
                gap = held(j) - o

                @pl.when(((gap == w) | (gap == -w)) & when)
                def _():
                    lines_in(j)

    def relay(j):
        for a in range(2):
            side(j, a, nbr[a]).wait_recv()
            if j == 0:
                diag(0, a, nbr[a]).start()
            share_all(j, 1 + a)

    def relay_diag():
        for a in range(2):
            diag(0, a, ixy).wait_recv()
            share_all(0, 3 + a)
        for j in range(1, n_o):
            cross(j, o).start()

    def cross_in(j):
        cross(j, held(j)).wait_recv()
        share_all(j, 3)

    def shares_in(j, *kinds):
        for k in kinds:
            if j > 0 or k > 0:
                for e in range(1, tp):
                    share(e, j, k, lax.rem(t + tp - e, tp)).wait_recv()

    for copy in first[5:]:
        copy.wait()
    for load in loads:
        load.start()
    for a in range(2):
        side(0, a, i).start()
    line_send(o)
    for d in range(1, tp):
        own_copy(d, t).start()

    lat_out[n_lat - GRID_W :, :] = jnp.zeros((GRID_W, width), jnp.bfloat16)

    @pl.when(s == 0)
    def _():
        lat_out[:halo, :] = jnp.zeros((halo, width), jnp.bfloat16)

    @pl.when(s == sp - 1)
    def _():
        lat_out[halo + tokens : n_lat - GRID_W, :] = jnp.zeros(
            (halo - GRID_W, width), jnp.bfloat16
        )

    def build_bias(low, high):
        grid_rows = tokens // GRID_W
        lanes = lax.broadcasted_iota(jnp.int32, (GRID_W, 128), 1)
        cq = lax.broadcasted_iota(jnp.int32, (GRID_W, 128), 0)
        c2 = lax.rem(lanes, GRID_W)
        group = lanes // GRID_W
        cs = jnp.clip(cq - WIN_W // 2, 0, GRID_W - WIN_W)
        col_in = (c2 >= cs) & (c2 < cs + WIN_W)
        per = 128 // GRID_W
        start = s * grid_rows
        kr = lax.broadcasted_iota(jnp.int32, (GRID_W, n_lat), 1) // GRID_W

        def body(h, c):
            v_buf[:, pl.ds(pl.multiple_of(h * 2 * HEAD_DIM + HEAD_DIM, HEAD_DIM), HEAD_DIM)] = (
                jnp.ones((v_buf.shape[0], HEAD_DIM), jnp.bfloat16)
            )
            groups = []
            for k in range(24 // per):
                part = jnp.full((GRID_W, 128), NEG_BIG, jnp.float32)
                for g in range(per):
                    if not HALF <= per * k + g < HALF + tab_ref.shape[0]:
                        continue
                    row = tab_ref[per * k + g - HALF, pl.ds(t * heads + h, 1), :] * LOG2E
                    row = jnp.concatenate(
                        [row, jnp.zeros((1, LANES - row.shape[1]), jnp.float32)], axis=1
                    )
                    rolled = pltpu.roll(
                        jnp.broadcast_to(row, (GRID_W, 128)),
                        (GRID_W * g - (WIN_W - 1)) % 128, 1, stride=1, stride_axis=0,
                    )
                    part = jnp.where(group == g, rolled, part)
                groups.append(jnp.where(col_in, part, NEG_BIG))
            table = jnp.concatenate(groups, axis=1)
            total = table.shape[1]
            for r in range(grid_rows):
                shift = (grid_rows - 1 - r) * GRID_W
                strip = table if shift == 0 else pltpu.roll(table, total - shift, 1)
                lo = jnp.clip(start + r - HALF, 0, grid_rows * sp - WIN_H) - start + HALF
                bias[h, r * GRID_W : (r + 1) * GRID_W, :] = jnp.where(
                    (kr >= lo) & (kr < lo + WIN_H), strip[:, :n_lat], NEG_BIG
                )
            return c

        lax.fori_loop(low, high, body, 0, unroll=min(2, high - low))

    build_bias(0, heads // 2)
    for d in range(1, INNER):
        mod_in(d, i).wait_send()
    for d in range(1, INNER):
        mod_in(d, lax.rem(i + INNER - d, INNER)).wait_recv()
    out_buf[pl.ds(o, 1)] = jnp.sum(in_buf[...], axis=0, keepdims=True)
    for d in range(1, n_o):
        mod_across(d, o).start()
    halo_start(0)
    build_bias(heads // 2, heads)
    relay(0)
    lines_wave([1])
    halo_start(1)

    for d in range(1, n_o):
        mod_across(d, o).wait_send()
    for d in range(1, n_o):
        mod_across(d, lax.rem(o + n_o - d, n_o)).wait_recv()
    mod_out[pl.ds(t, 1)] = jnp.sum(out_buf[...], axis=0, keepdims=True)
    for d in range(1, tp):
        mod_fwd(d, t).start()
    for d in range(1, tp):
        own_copy(d, lax.rem(t + tp - d, tp)).wait_recv()
    for d in range(1, tp):
        mod_fwd(d, lax.rem(t + tp - d, tp)).wait_recv()
    for w in range(tp):
        for c in range(n_piece):
            low = w * mod_cols + c * LANES
            cut = slice(low, low + LANES)
            for kind in range(2):
                r = VECS * c + kind
                affine[2 * kind : 2 * kind + 1, cut] = gain_ref[:, cut] * (
                    1.0 + mod_out[w, r + 2 : r + 3, :]
                )
                affine[2 * kind + 1 : 2 * kind + 2, cut] = mod_out[w, r : r + 1, :]
            gate[:, cut] = mod_out[w, VECS * c + 4 : VECS * c + 5, :]

    def norm_piece(src, src_row, dst, dst_row, count, kind):
        x = src[pl.ds(src_row, count), :].astype(jnp.float32)
        r = lax.rsqrt(jnp.mean(x * x, axis=1, keepdims=True) + NORM_EPS)
        y = x * r * affine[2 * kind : 2 * kind + 1, :] + affine[2 * kind + 1 : 2 * kind + 2, :]
        dst[dst_row : dst_row + count, :] = y.astype(jnp.bfloat16)

    STEP = 16

    def normalise(pieces, dst, kind, low=0):
        todo = []
        for src, row, size in pieces:
            for k in range(0, size, STEP):
                at_row = row + k
                if not isinstance(at_row, int):
                    at_row = pl.multiple_of(at_row, STEP)
                todo.append(
                    functools.partial(norm_piece, src, at_row, dst, low + k, STEP, kind)
                )
            low += size
        return todo

    def project(src, w, dst, pieces, scale=None, spread=1):
        count = sum(p[1] for p in pieces)
        cc = 2 * HEAD_DIM

        def one(n):
            y = jnp.dot(
                src[:count, :], w[:, n * cc : (n + 1) * cc], preferred_element_type=jnp.float32
            )
            if scale is not None:
                y = y * scale
            y = y.astype(jnp.bfloat16)
            low = 0
            for start, size in pieces:
                if spread == 1:
                    dst[start : start + size, n * cc : (n + 1) * cc] = y[low : low + size]
                else:
                    for k in range(2):
                        col = (2 * n + k) * cc
                        dst[start : start + size, col : col + HEAD_DIM] = y[
                            low : low + size, k * HEAD_DIM : (k + 1) * HEAD_DIM
                        ]
                low += size

        return [functools.partial(one, n) for n in range(cols // cc)]

    def run(dots, norms=()):
        done = 0
        for n, dot in enumerate(dots):
            dot()
            upto = (n + 1) * len(norms) // len(dots)
            for norm in norms[done:upto]:
                norm()
            done = upto
        for norm in norms[done:]:
            norm()

    part_rows = n_o * crow
    own = ((halo, tokens),)
    ends = ((0, halo), (halo + tokens, halo))
    planes = range(n_o)

    order = sorted(
        [(c, j) for c in range(INNER) for j in planes],
        key=lambda u: max(u[1] - 1, 0) if u[0] == 0 else u[1] + u[0] // 3,
    )

    def units(c):
        return order[c * n_o : (c + 1) * n_o]

    def norm_ctx(c, dst, low=0, high=n_o):
        todo = []
        for k, (col, j) in list(enumerate(units(c)))[low:high]:
            at_row = (held(j) * INNER + (i, ix, iy, ixy)[col]) * crow
            todo += normalise([(ctx_out, at_row, crow)], dst, 1, k * crow)
        return todo

    def arrived(c, low=0, high=n_o):
        for col, j in units(c)[low:high]:
            shares_in(j, *((col,) if col < 3 or j > 0 else (3, 4)))

    def ctx_at(c):
        return ((n_lat + c * part_rows, part_rows),)

    def k_of(src, pieces):
        return project(src, wk, k_buf, pieces)

    def v_of(src, pieces):
        return project(src, wv, v_buf, pieces, spread=2)

    halo_norm = normalise([(lat_out, 0, halo), (lat_out, halo + tokens, halo)], nbuf0, 0)
    inner_plane = jnp.logical_not(outer_plane)
    passed = range(1, n_o - 2)

    run([], normalise([(lat_out, halo, tokens)], nbuf0, 0))
    loads[0].wait()
    run(project(nbuf0, wq, q_buf, ((0, tokens),), HEAD_DIM ** -0.5 * LOG2E))
    lines_wave(planes[2 : n_o - 1], inner_plane)
    relay_diag()
    loads[1].wait()
    run(k_of(nbuf0, own))
    lines_wave(planes[2 : n_o - 1], outer_plane)
    for p in range(2, rows // GRID_W):
        halo_start(p)
    arrived(0)
    loads[2].wait()
    run(v_of(nbuf0, own), norm_ctx(0, nbuf1))
    for j in passed:
        relay(j)
    run(k_of(nbuf1, ctx_at(0)))
    arrived(1)
    run(v_of(nbuf1, ctx_at(0)), norm_ctx(1, nbuf0))
    relay(n_o - 2)
    run(k_of(nbuf0, ctx_at(1)))
    lines_wave(planes[n_o - 1 :])
    for j in passed:
        cross_in(j)
    run(v_of(nbuf0, ctx_at(1)))
    arrived(2)
    run([], norm_ctx(2, nbuf1))
    run(k_of(nbuf1, ctx_at(2)))
    halo_relay()
    relay(n_o - 1)
    run(v_of(nbuf1, ctx_at(2)))
    for j in planes[n_o - 2 :]:
        cross_in(j)
    halo_in()
    run([], halo_norm)
    run(k_of(nbuf0, ends))
    arrived(3)
    run(v_of(nbuf0, ends), norm_ctx(3, nbuf1))
    run(k_of(nbuf1, ctx_at(3)) + v_of(nbuf1, ctx_at(3)))

    n_all = k_buf.shape[0]

    def attend(h, c):
        cut = pl.ds(pl.multiple_of(h * HEAD_DIM, HEAD_DIM), HEAD_DIM)

        def scores(start, count):
            return lax.dot_general(
                q_buf[:, cut], k_buf[pl.ds(start, count), cut],
                (((1,), (1,)), ((), ())), preferred_element_type=jnp.float32,
            )

        win = scores(0, n_lat) + bias[h]
        ctx = scores(n_lat, n_all - n_lat)
        m = jnp.maximum(jnp.max(win, axis=1, keepdims=True), jnp.max(ctx, axis=1, keepdims=True))
        e = jnp.concatenate(
            [jnp.exp2(win - m).astype(jnp.bfloat16), jnp.exp2(ctx - m).astype(jnp.bfloat16)],
            axis=1,
        )
        y = jnp.dot(
            e, v_buf[:, pl.ds(pl.multiple_of(h * 2 * HEAD_DIM, 2 * HEAD_DIM), 2 * HEAD_DIM)],
            preferred_element_type=jnp.float32,
        )
        att[:, cut] = (y[:, :HEAD_DIM] / y[:, HEAD_DIM:]).astype(jnp.bfloat16)
        return c

    lax.fori_loop(0, heads, attend, 0, unroll=heads)

    loads[3].wait()
    n_chunk = ybuf.shape[0]
    ow = ybuf.shape[2]

    def part(c, who):
        return ybuf.at[c, pl.ds(pl.multiple_of(who * rows, rows), rows), :]

    def swap(d, c):
        return remote(
            part(c, tp_peer(d)), rbuf.at[d, c], x_send.at[d, c], x_recv.at[d, c],
            (s, tp_peer(d)),
        )

    def leave(c):
        cut = pl.ds(c * ow, ow)
        return pltpu.make_async_copy(out_ref.at[:, cut], out_hbm.at[:, cut], out_sem.at[c])

    for c in range(n_chunk):
        ybuf[c] = jnp.dot(
            att[...], wo[:, c * ow : (c + 1) * ow], preferred_element_type=jnp.float32
        ).astype(jnp.bfloat16)
        for d in range(1, tp):
            swap(d, c).start()
    for c in range(n_chunk):
        branch = part(c, t)[...].astype(jnp.float32)
        for d in range(1, tp):
            swap(d, c).wait_recv()
            branch = branch + rbuf[d, c].astype(jnp.float32)
        sl = slice(c * ow, (c + 1) * ow)
        mine = lat_out[pl.ds(pl.multiple_of(halo + t * rows, rows), rows), sl]
        out_ref[:, sl] = (mine.astype(jnp.float32) + gate[:, sl] * branch).astype(jnp.bfloat16)
        leave(c).start()

    for d in range(1, tp):
        own_copy(d, t).wait_send()
        mod_fwd(d, t).wait_send()
        for c in range(n_chunk):
            swap(d, c).wait_send()
    halo_drain()
    for j in range(n_o):
        for k in range(4 if j else 5):
            if j == 0 and k == 0:
                continue
            for e in range(1, tp):
                share(e, j, k, t).wait_send()
        for a in range(2):
            side(j, a, i).wait_send()
            if j == 0:
                diag(0, a, nbr[a]).wait_send()
    for j in range(n_o):
        line_drain(held(j))
        if j > 0:
            cross(j, o).wait_send()
    for c in range(n_chunk):
        leave(c).wait()


def layer(sp, tp, vmem, cond, cctx, gain, table, *big):
    w_shift, latent, context, w_query = big[0], big[3], big[4], big[5]
    rows, width = latent.shape
    row_part, mod_cols = w_shift.shape
    cols = w_query.shape[1]
    heads = cols // HEAD_DIM
    tokens = rows * tp
    n_lat = 2 * tokens
    n_ctx = context.shape[0] * sp
    n_o = sp // INNER
    n_chunk = max(4, tp)
    pack = -(-VECS * (mod_cols // LANES) // 8) * 8
    dma = pltpu.SemaphoreType.DMA
    spec = pl.BlockSpec(memory_space=pltpu.HBM)
    bf, f32 = jnp.bfloat16, jnp.float32
    pieces = rows // GRID_W
    step_rows = max(tokens, n_ctx // INNER)
    return pl.pallas_call(
        functools.partial(layer_kernel, sp, tp),
        out_shape=jax.ShapeDtypeStruct(latent.shape, bf),
        in_specs=[spec] * 13,
        out_specs=spec,
        scratch_shapes=[
            VMEM(cond.shape, f32), VMEM(cctx.shape, f32), VMEM(gain.shape, f32),
            VMEM(table.shape, f32), VMEM(latent.shape, bf), dma((n_chunk,)),
            VMEM((row_part, mod_cols), bf), VMEM((row_part, mod_cols), bf),
            VMEM((row_part, mod_cols), bf),
            VMEM((tp, pack, LANES), f32),
            VMEM((n_lat, width), bf),
            VMEM((n_ctx, width), bf),
            VMEM((width, cols), bf), VMEM((width, cols), bf), VMEM((width, cols), bf),
            VMEM((cols, width), bf),
            VMEM((8, width), f32), VMEM((1, width), f32),
            VMEM((step_rows, width), bf), VMEM((step_rows, width), bf),
            VMEM((tokens, cols), bf),
            VMEM((n_lat + n_ctx, cols), bf), VMEM((n_lat + n_ctx, 2 * cols), bf),
            VMEM((heads, tokens, n_lat), f32),
            VMEM((tokens, cols), bf),
            VMEM((n_chunk, tokens, width // n_chunk), bf),
            VMEM((tp, n_chunk, rows, width // n_chunk), bf),
            dma((9,)), dma((4,)), dma((tp, n_chunk)), dma((tp, n_chunk)),
            VMEM((INNER, pack, LANES), f32),
            VMEM((n_o, pack, LANES), f32),
            dma((INNER,)), dma((INNER,)), dma((n_o,)), dma((n_o,)), dma((tp,)), dma((tp,)),
            dma((tp,)), dma((tp,)), dma((pieces,)), dma((pieces,)),
            dma((tp, pieces)), dma((tp, pieces)),
            dma((n_o, 2)), dma((n_o,)), dma((n_o,)), dma((n_o,)),
            dma((n_o, 2)), dma((n_o, 2)), dma((1, 2)), dma((1, 2)), dma((tp, n_o, 5)), dma((tp, n_o, 5)),
        ],
        compiler_params=pltpu.CompilerParams(
            collective_id=0, has_side_effects=True, vmem_limit_bytes=vmem
        ),
        name="layer",
    )(cond, cctx, gain, table, *big)


def on_device(
    latent, context, condition, ctx_cond, norm_gain, w_shift, w_scale, w_gate,
    w_query, w_key, w_value, w_out, rel_bias,
):
    tp = lax.axis_size("tp")
    sp = lax.axis_size("sp")
    tokens = latent.shape[0] * tp
    halo = HALF * GRID_W
    assert tokens == 2 * halo and tp % 2 == 0 and sp % (4 * INNER) == 0
    return layer(
        sp, tp, 55 * 1024 * 1024, condition[None], ctx_cond[None], norm_gain[None],
        jnp.transpose(rel_bias, (1, 0, 2)),
        w_shift, w_scale, w_gate, latent, context, w_query, w_key, w_value, w_out,
    )


def solution(mesh):
    placed = (
        P(("sp", "tp"), None),
        P("sp", None),
        P(),
        P(),
        P(),
        P("sp", "tp"),
        P("sp", "tp"),
        P("sp", "tp"),
        P(None, "tp"),
        P(None, "tp"),
        P(None, "tp"),
        P("tp", None),
        P(),
    )
    return jax.shard_map(
        on_device, mesh=mesh, in_specs=placed, out_specs=P(("sp", "tp"), None), check_vma=False
    )
```

```python
import functools

import jax
import jax.numpy as jnp
from jax import lax
from jax.experimental import pallas as pl
from jax.experimental.pallas import tpu as pltpu
from jax.sharding import PartitionSpec as P

HEAD_DIM = 128
GRID_W = 32
WIN_H = 8
WIN_W = 16
HALF = WIN_H // 2
INNER = 4
VECS = 5
LANES = 128
NORM_EPS = 1e-06
NEG_BIG = -1e30
LOG2E = 1.4426950408889634
MESH = pl.DeviceIdType.MESH
VMEM = pltpu.VMEM


def layer_kernel(
    sp, tp, cond_hbm, cctx_hbm, gain_hbm, tab_hbm,
    wsh_hbm, wsc_hbm, wg_hbm, lat_hbm, ctx_hbm, wq_hbm, wk_hbm, wv_hbm, wo_hbm,
    out_hbm,
    cond_ref, cctx_ref, gain_ref, tab_ref, out_ref, out_sem, wsh, wsc, wg, mod_out, lat_out, ctx_out, wq, wk, wv, wo, affine, gate, nbuf0, nbuf1,
    q_buf, k_buf, v_buf, bias, att, ybuf, rbuf,
    in_sem, w_sem, x_send, x_recv,
    in_buf, out_buf, mi_send, mi_recv, mo_send, mo_recv, mf_send, mf_recv,
    own_send, own_recv, h_send, h_recv, hf_send, hf_recv,
    z_send, z_recv, c_send, c_recv, n_send, n_recv, d_send, d_recv, f_send, f_recv,
):
    s = lax.axis_index("sp")
    t = lax.axis_index("tp")
    n_o = sp // INNER
    o = s // INNER
    i = lax.rem(s, INNER)
    rows, width = lat_hbm.shape
    crow = ctx_hbm.shape[0]
    cw = width // tp
    hw = max(LANES, 3 * cw // 4 // LANES * LANES)
    tokens = rows * tp
    halo = tokens // 2
    n_lat = 2 * tokens
    cols = wq.shape[1]
    heads = cols // HEAD_DIM
    mod_cols = wsh.shape[1]
    n_piece = mod_cols // LANES

    def remote(src, dst, ss, rs, dev):
        return pltpu.make_async_remote_copy(
            src_ref=src, dst_ref=dst, send_sem=ss, recv_sem=rs,
            device_id=dev, device_id_type=MESH,
        )

    def at(oo, ii):
        return (oo * INNER + ii, t)

    def held(j):
        if j == 0:
            return o
        low, high = o, n_o - 1 - o
        both = jnp.minimum(low, high)
        step = (j + 1) // 2
        near = o - step if j % 2 else o + step
        far = jnp.where(low < high, o + (j - both), o - (j - both))
        return jnp.where(j <= 2 * both, near, far)

    def outer(d):
        return lax.rem(o + d, n_o)

    def inner(d):
        return lax.rem(i + d, INNER)

    def tp_peer(d):
        return lax.rem(t + d, tp)

    ix = i + 1 - 2 * lax.rem(i, 2)
    iy = lax.rem(i + 2, INNER)
    ixy = lax.rem(ix + 2, INNER)
    nbr = (ix, iy)
    nxt = lax.rem(s + 1, sp)
    prv = lax.rem(s + sp - 1, sp)

    barrier = pltpu.get_barrier_semaphore()

    def greet(dev):
        pl.semaphore_signal(barrier, inc=1, device_id=dev, device_id_type=MESH)

    for d in range(1, n_o):
        greet(at(outer(d), i))
    for d in range(1, INNER):
        greet(at(o, inner(d)))
    for d in range(1, tp):
        greet((s, tp_peer(d)))
    for way, to in ((s < sp - 1, nxt), (s > 0, prv)):
        @pl.when(way)
        def _():
            greet((to, t))

    def own_rows(who):
        return lat_out.at[pl.ds(pl.multiple_of(halo + who * rows, rows), rows), :]

    first = [
        pltpu.make_async_copy(src, dst, in_sem.at[n])
        for n, (src, dst) in enumerate(
            (
                (cond_hbm, cond_ref), (cctx_hbm, cctx_ref),
                (wsh_hbm, wsh), (wsc_hbm, wsc), (wg_hbm, wg),
                (gain_hbm, gain_ref), (tab_hbm, tab_ref),
                (ctx_hbm, ctx_out.at[pl.ds(pl.multiple_of(s * crow, crow), crow), :]),
                (lat_hbm, own_rows(t)),
            )
        )
    ]
    loads = [
        pltpu.make_async_copy(src, dst, w_sem.at[n])
        for n, (src, dst) in enumerate(
            ((wq_hbm, wq), (wk_hbm, wk), (wv_hbm, wv), (wo_hbm, wo))
        )
    ]
    for copy in first:
        copy.start()

    row_part = wsh.shape[0]
    begin = s * row_part

    def act_of(ref):
        if row_part % LANES == 0:
            x = ref[:, pl.ds(pl.multiple_of(begin, LANES), row_part)]
            x = jnp.broadcast_to(x, (8, row_part))
        else:
            base = begin // LANES * LANES
            x = jnp.broadcast_to(ref[:, pl.ds(pl.multiple_of(base, LANES), LANES)], (8, LANES))
            x = pltpu.roll(x, lax.rem(LANES - (begin - base), LANES), 1)[:, :row_part]
        return x * jax.nn.sigmoid(x)

    for copy in first[:5]:
        copy.wait()
    act_a, act_c = act_of(cond_ref), act_of(cctx_ref)
    sub = lax.broadcasted_iota(jnp.int32, (8, row_part), 0)

    def act(k):
        both = jnp.where(sub == 2 * k, act_a, 0.0)
        if k < 2:
            both = jnp.where(sub == 2 * k + 1, act_c, both)
        return both.astype(jnp.bfloat16)

    val = (
        jnp.dot(act(0), wsh[...], preferred_element_type=jnp.float32)
        + jnp.dot(act(1), wsc[...], preferred_element_type=jnp.float32)
        + jnp.dot(act(2), wg[...], preferred_element_type=jnp.float32)
    )
    for c in range(n_piece):
        in_buf[pl.ds(i, 1), VECS * c : VECS * (c + 1), :] = val[
            :VECS, c * LANES : (c + 1) * LANES
        ][None]

    ends_met = jnp.where(s == 0, 1, 0) + jnp.where(s == sp - 1, 1, 0)
    pl.semaphore_wait(barrier, n_o - 1 + INNER - 1 + tp - 1 + 2 - ends_met)

    def mod_in(d, who):
        return remote(
            in_buf.at[who], in_buf.at[who], mi_send.at[d], mi_recv.at[d], at(o, inner(d))
        )

    def mod_across(d, who):
        return remote(
            out_buf.at[who], out_buf.at[who], mo_send.at[d], mo_recv.at[d], at(outer(d), i)
        )

    def mod_fwd(d, who):
        return remote(
            mod_out.at[who], mod_out.at[who], mf_send.at[d], mf_recv.at[d], (s, tp_peer(d))
        )

    for d in range(1, INNER):
        mod_in(d, i).start()

    def own_copy(d, who):
        return remote(
            own_rows(who), own_rows(who), own_send.at[d], own_recv.at[d], (s, tp_peer(d))
        )

    halos = []
    for who in range(tp):
        down = who >= tp // 2
        for p in range(rows // GRID_W):
            low = who * rows + p * GRID_W
            if down:
                off = low - halo
            elif low < (HALF - 1) * GRID_W:
                off = halo + tokens + low
            else:
                continue
            halos.append(
                (
                    p, who, halo + low, off, (nxt, t) if down else (prv, t),
                    (s < sp - 1) if down else (s > 0), (s > 0) if down else (s < sp - 1),
                )
            )

    def halo_copy(p, low, off, dev):
        return remote(
            lat_out.at[pl.ds(low, GRID_W), :], lat_out.at[pl.ds(off, GRID_W), :],
            h_send.at[p], h_recv.at[p], dev,
        )

    def halo_fwd(p, who, off, e):
        ref = lat_out.at[pl.ds(off, GRID_W), :]
        return remote(ref, ref, hf_send.at[e, p], hf_recv.at[who, p], (s, tp_peer(e)))

    def halo_start(piece, far):
        for p, who, low, off, dev, gives, takes in halos:
            edge = i == (INNER - 1 if who >= tp // 2 else 0)
            if p == piece:
                @pl.when((t == who) & gives & (edge if far else jnp.logical_not(edge)))
                def _():
                    halo_copy(p, low, off, dev).start()

    def halo_relay():
        for p, who, low, off, dev, gives, takes in halos:
            @pl.when((t == who) & takes)
            def _():
                halo_copy(p, low, off, dev).wait_recv()
                for e in range(1, tp):
                    halo_fwd(p, who, off, e).start()

    def halo_in():
        for p, who, low, off, dev, gives, takes in halos:
            @pl.when((t != who) & takes)
            def _():
                halo_fwd(p, who, off, 1).wait_recv()

    def halo_drain():
        for p, who, low, off, dev, gives, takes in halos:
            @pl.when((t == who) & gives)
            def _():
                halo_copy(p, low, off, dev).wait_send()

            @pl.when((t == who) & takes)
            def _():
                for e in range(1, tp):
                    halo_fwd(p, who, off, e).wait_send()

    def block(oo, ii, who, half=None):
        low, size = ((0, cw), (0, hw), (hw, cw - hw))[0 if half is None else half + 1]
        return ctx_out.at[
            pl.ds(pl.multiple_of((oo * INNER + ii) * crow, crow), crow),
            pl.ds(pl.multiple_of(who * cw + low, LANES), size),
        ]

    def line(src, way):
        ref = block(src, i, t)
        to = jnp.clip(o + 2 * way - 1, 0, n_o - 1)
        return remote(ref, ref, z_send.at[src, way], z_recv.at[src], at(to, i))

    def onward(src, way):
        return (src <= o) & (o < n_o - 1) if way else (src >= o) & (o > 0)

    def line_send(src):
        for way in range(2):
            @pl.when(onward(src, way))
            def _():
                line(src, way).start()

    def cross(j, src):
        ref = block(src, ixy, t)
        return remote(ref, ref, c_send.at[j], c_recv.at[src], at(held(j), i))

    def line_drain(src):
        for way in range(2):
            @pl.when(onward(src, way))
            def _():
                line(src, way).wait_send()

    def side(j, a, ii):
        ref = block(held(j), ii, t)
        return remote(ref, ref, n_send.at[j, a], n_recv.at[j, a], at(o, nbr[a]))

    def diag(j, a, ii):
        ref = block(held(j), ii, t, a)
        return remote(ref, ref, d_send.at[j, a], d_recv.at[j, a], at(o, nbr[1 - a]))

    def share(e, j, k, who):
        half = None if k < 3 or j > 0 else k - 3
        ref = block(held(j), (i, ix, iy, ixy, ixy)[k], who, half)
        return remote(
            ref, ref, f_send.at[e, j, k], f_recv.at[e, j, k], (s, tp_peer(e))
        )

    def share_all(j, k):
        for e in range(1, tp):
            share(e, j, k, t).start()

    def lines_in(j):
        line(held(j), 0).wait_recv()
        line_send(held(j))
        for a in range(2):
            side(j, a, i).start()
        share_all(j, 0)

    outer_plane = (o == 0) | (o == n_o - 1)

    def lines_wave(far, when=True):
        for w in far:
            for j in range(1, n_o):
                gap = held(j) - o

                @pl.when(((gap == w) | (gap == -w)) & when)
                def _():
                    lines_in(j)

    def relay(j):
        for a in range(2):
            side(j, a, nbr[a]).wait_recv()
            if j == 0:
                diag(0, a, nbr[a]).start()
            share_all(j, 1 + a)

    def relay_diag():
        for a in range(2):
            diag(0, a, ixy).wait_recv()
            share_all(0, 3 + a)
        for j in range(1, n_o):
            cross(j, o).start()

    def cross_in(j):
        cross(j, held(j)).wait_recv()
        share_all(j, 3)

    def shares_in(j, *kinds):
        for k in kinds:
            if j > 0 or k > 0:
                for e in range(1, tp):
                    share(e, j, k, lax.rem(t + tp - e, tp)).wait_recv()

    for copy in first[5:]:
        copy.wait()
    for load in loads:
        load.start()
    for a in range(2):
        side(0, a, i).start()
    line_send(o)
    for d in range(1, tp):
        own_copy(d, t).start()

    lat_out[n_lat - GRID_W :, :] = jnp.zeros((GRID_W, width), jnp.bfloat16)

    @pl.when(s == 0)
    def _():
        lat_out[:halo, :] = jnp.zeros((halo, width), jnp.bfloat16)

    @pl.when(s == sp - 1)
    def _():
        lat_out[halo + tokens : n_lat - GRID_W, :] = jnp.zeros(
            (halo - GRID_W, width), jnp.bfloat16
        )

    def build_bias(low, high):
        grid_rows = tokens // GRID_W
        lanes = lax.broadcasted_iota(jnp.int32, (GRID_W, 128), 1)
        cq = lax.broadcasted_iota(jnp.int32, (GRID_W, 128), 0)
        c2 = lax.rem(lanes, GRID_W)
        group = lanes // GRID_W
        cs = jnp.clip(cq - WIN_W // 2, 0, GRID_W - WIN_W)
        col_in = (c2 >= cs) & (c2 < cs + WIN_W)
        per = 128 // GRID_W
        start = s * grid_rows
        kr = lax.broadcasted_iota(jnp.int32, (GRID_W, n_lat), 1) // GRID_W

        def body(h, c):
            v_buf[:, pl.ds(pl.multiple_of(h * 2 * HEAD_DIM + HEAD_DIM, HEAD_DIM), HEAD_DIM)] = (
                jnp.ones((v_buf.shape[0], HEAD_DIM), jnp.bfloat16)
            )
            groups = []
            for k in range(24 // per):
                part = jnp.full((GRID_W, 128), NEG_BIG, jnp.float32)
                for g in range(per):
                    if not HALF <= per * k + g < HALF + tab_ref.shape[0]:
                        continue
                    row = tab_ref[per * k + g - HALF, pl.ds(t * heads + h, 1), :] * LOG2E
                    row = jnp.concatenate(
                        [row, jnp.zeros((1, LANES - row.shape[1]), jnp.float32)], axis=1
                    )
                    rolled = pltpu.roll(
                        jnp.broadcast_to(row, (GRID_W, 128)),
                        (GRID_W * g - (WIN_W - 1)) % 128, 1, stride=1, stride_axis=0,
                    )
                    part = jnp.where(group == g, rolled, part)
                groups.append(jnp.where(col_in, part, NEG_BIG))
            table = jnp.concatenate(groups, axis=1)
            total = table.shape[1]
            for r in range(grid_rows):
                shift = (grid_rows - 1 - r) * GRID_W
                strip = table if shift == 0 else pltpu.roll(table, total - shift, 1)
                lo = jnp.clip(start + r - HALF, 0, grid_rows * sp - WIN_H) - start + HALF
                bias[h, r * GRID_W : (r + 1) * GRID_W, :] = jnp.where(
                    (kr >= lo) & (kr < lo + WIN_H), strip[:, :n_lat], NEG_BIG
                )
            return c

        lax.fori_loop(low, high, body, 0, unroll=min(2, high - low))

    build_bias(0, heads // 2)
    for d in range(1, INNER):
        mod_in(d, i).wait_send()
    for d in range(1, INNER):
        mod_in(d, lax.rem(i + INNER - d, INNER)).wait_recv()
    out_buf[pl.ds(o, 1)] = jnp.sum(in_buf[...], axis=0, keepdims=True)
    for d in range(1, n_o):
        mod_across(d, o).start()
    halo_start(0, False)
    halo_start(0, True)
    build_bias(heads // 2, heads)
    relay(0)
    lines_wave([1])
    halo_start(1, False)
    for p in range(1, rows // GRID_W):
        halo_start(p, True)

    for d in range(1, n_o):
        mod_across(d, o).wait_send()
    for d in range(1, n_o):
        mod_across(d, lax.rem(o + n_o - d, n_o)).wait_recv()
    mod_out[pl.ds(t, 1)] = jnp.sum(out_buf[...], axis=0, keepdims=True)
    for d in range(1, tp):
        mod_fwd(d, t).start()
    for d in range(1, tp):
        own_copy(d, lax.rem(t + tp - d, tp)).wait_recv()
    for d in range(1, tp):
        mod_fwd(d, lax.rem(t + tp - d, tp)).wait_recv()
    for w in range(tp):
        for c in range(n_piece):
            low = w * mod_cols + c * LANES
            cut = slice(low, low + LANES)
            for kind in range(2):
                r = VECS * c + kind
                affine[2 * kind : 2 * kind + 1, cut] = gain_ref[:, cut] * (
                    1.0 + mod_out[w, r + 2 : r + 3, :]
                )
                affine[2 * kind + 1 : 2 * kind + 2, cut] = mod_out[w, r : r + 1, :]
            gate[:, cut] = mod_out[w, VECS * c + 4 : VECS * c + 5, :]

    def norm_piece(src, src_row, dst, dst_row, count, kind):
        x = src[pl.ds(src_row, count), :].astype(jnp.float32)
        r = lax.rsqrt(jnp.mean(x * x, axis=1, keepdims=True) + NORM_EPS)
        y = x * r * affine[2 * kind : 2 * kind + 1, :] + affine[2 * kind + 1 : 2 * kind + 2, :]
        dst[dst_row : dst_row + count, :] = y.astype(jnp.bfloat16)

    STEP = 16

    def normalise(pieces, dst, kind, low=0):
        todo = []
        for src, row, size in pieces:
            for k in range(0, size, STEP):
                at_row = row + k
                if not isinstance(at_row, int):
                    at_row = pl.multiple_of(at_row, STEP)
                todo.append(
                    functools.partial(norm_piece, src, at_row, dst, low + k, STEP, kind)
                )
            low += size
        return todo

    def project(src, w, dst, pieces, scale=None, spread=1):
        count = sum(p[1] for p in pieces)
        cc = 2 * HEAD_DIM

        def one(n):
            y = jnp.dot(
                src[:count, :], w[:, n * cc : (n + 1) * cc], preferred_element_type=jnp.float32
            )
            if scale is not None:
                y = y * scale
            y = y.astype(jnp.bfloat16)
            low = 0
            for start, size in pieces:
                if spread == 1:
                    dst[start : start + size, n * cc : (n + 1) * cc] = y[low : low + size]
                else:
                    for k in range(2):
                        col = (2 * n + k) * cc
                        dst[start : start + size, col : col + HEAD_DIM] = y[
                            low : low + size, k * HEAD_DIM : (k + 1) * HEAD_DIM
                        ]
                low += size

        return [functools.partial(one, n) for n in range(cols // cc)]

    def run(dots, norms=()):
        done = 0
        for n, dot in enumerate(dots):
            dot()
            upto = (n + 1) * len(norms) // len(dots)
            for norm in norms[done:upto]:
                norm()
            done = upto
        for norm in norms[done:]:
            norm()

    own = ((halo, tokens),)
    ends = ((0, halo), (halo + tokens, halo))
    planes = range(n_o)

    order = sorted(
        [(c, j) for c in range(INNER) for j in planes],
        key=lambda u: max(u[1] - 1, 0) if u[0] == 0 else u[1] + u[0] // 3 * (n_o if u[1] else 1),
    )
    bounds = (0, n_o, 2 * n_o, 3 * n_o - 1, 4 * n_o)

    def units(c):
        return order[bounds[c] : bounds[c + 1]]

    def norm_ctx(c, dst):
        todo = []
        for k, (col, j) in enumerate(units(c)):
            at_row = (held(j) * INNER + (i, ix, iy, ixy)[col]) * crow
            todo += normalise([(ctx_out, at_row, crow)], dst, 1, k * crow)
        return todo

    def arrived(c):
        for col, j in units(c):
            shares_in(j, *((col,) if col < 3 or j > 0 else (3, 4)))

    def ctx_at(c):
        return ((n_lat + bounds[c] * crow, (bounds[c + 1] - bounds[c]) * crow),)

    def k_of(src, pieces):
        return project(src, wk, k_buf, pieces)

    def v_of(src, pieces):
        return project(src, wv, v_buf, pieces, spread=2)

    halo_norm = normalise([(lat_out, 0, halo), (lat_out, halo + tokens, halo)], nbuf0, 0)
    inner_plane = jnp.logical_not(outer_plane)
    passed = range(1, n_o - 2)

    run([], normalise([(lat_out, halo, tokens)], nbuf0, 0))
    loads[0].wait()
    run(project(nbuf0, wq, q_buf, ((0, tokens),), HEAD_DIM ** -0.5 * LOG2E))
    lines_wave(planes[2 : n_o - 1], inner_plane)
    relay_diag()
    loads[1].wait()
    run(k_of(nbuf0, own))
    lines_wave(planes[2 : n_o - 1], outer_plane)
    for p in range(2, rows // GRID_W):
        halo_start(p, False)
    arrived(0)
    loads[2].wait()
    run(v_of(nbuf0, own), norm_ctx(0, nbuf1))
    for j in passed:
        relay(j)
    run(k_of(nbuf1, ctx_at(0)))
    arrived(1)
    run(v_of(nbuf1, ctx_at(0)), norm_ctx(1, nbuf0))
    run(k_of(nbuf0, ctx_at(1)))
    relay(n_o - 2)
    lines_wave(planes[n_o - 1 :])
    run(v_of(nbuf0, ctx_at(1)))
    arrived(2)
    run([], norm_ctx(2, nbuf1))
    run(k_of(nbuf1, ctx_at(2)))
    halo_relay()
    run(v_of(nbuf1, ctx_at(2)))
    relay(n_o - 1)
    for j in planes[1:]:
        cross_in(j)
    halo_in()
    run([], halo_norm)
    run(k_of(nbuf0, ends))
    arrived(3)
    run(v_of(nbuf0, ends), norm_ctx(3, nbuf1))
    run(k_of(nbuf1, ctx_at(3)) + v_of(nbuf1, ctx_at(3)))

    n_all = k_buf.shape[0]

    def attend(h, c):
        cut = pl.ds(pl.multiple_of(h * HEAD_DIM, HEAD_DIM), HEAD_DIM)

        def scores(start, count):
            return lax.dot_general(
                q_buf[:, cut], k_buf[pl.ds(start, count), cut],
                (((1,), (1,)), ((), ())), preferred_element_type=jnp.float32,
            )

        win = scores(0, n_lat) + bias[h]
        ctx = scores(n_lat, n_all - n_lat)
        m = jnp.maximum(jnp.max(win, axis=1, keepdims=True), jnp.max(ctx, axis=1, keepdims=True))
        e = jnp.concatenate(
            [jnp.exp2(win - m).astype(jnp.bfloat16), jnp.exp2(ctx - m).astype(jnp.bfloat16)],
            axis=1,
        )
        y = jnp.dot(
            e, v_buf[:, pl.ds(pl.multiple_of(h * 2 * HEAD_DIM, 2 * HEAD_DIM), 2 * HEAD_DIM)],
            preferred_element_type=jnp.float32,
        )
        att[:, cut] = (y[:, :HEAD_DIM] / y[:, HEAD_DIM:]).astype(jnp.bfloat16)
        return c

    lax.fori_loop(0, heads, attend, 0, unroll=heads)

    loads[3].wait()
    first_cut = 3 * width // 4 // LANES * LANES
    cuts = ((0, first_cut), (first_cut, width - first_cut))
    n_chunk = len(cuts)

    def part(c, who):
        return ybuf.at[pl.ds(pl.multiple_of(who * rows, rows), rows), pl.ds(*cuts[c])]

    def swap(d, c):
        return remote(
            part(c, tp_peer(d)), rbuf.at[d, :, pl.ds(*cuts[c])], x_send.at[d, c], x_recv.at[d, c],
            (s, tp_peer(d)),
        )

    def leave(c):
        cut = pl.ds(*cuts[c])
        return pltpu.make_async_copy(out_ref.at[:, cut], out_hbm.at[:, cut], out_sem.at[c])

    for c in range(n_chunk):
        low, size = cuts[c]
        step = 4 * LANES
        for k in range(low, low + size, step):
            cut = slice(k, min(k + step, low + size))
            ybuf[:, cut] = jnp.dot(
                att[...], wo[:, cut], preferred_element_type=jnp.float32
            ).astype(jnp.bfloat16)
        for d in range(1, tp):
            swap(d, c).start()
    for c in range(n_chunk):
        branch = part(c, t)[...].astype(jnp.float32)
        for d in range(1, tp):
            swap(d, c).wait_recv()
            branch = branch + rbuf[d, :, cuts[c][0] : sum(cuts[c])].astype(jnp.float32)
        sl = slice(cuts[c][0], sum(cuts[c]))
        mine = lat_out[pl.ds(pl.multiple_of(halo + t * rows, rows), rows), sl]
        out_ref[:, sl] = (mine.astype(jnp.float32) + gate[:, sl] * branch).astype(jnp.bfloat16)
        leave(c).start()

    for d in range(1, tp):
        own_copy(d, t).wait_send()
        mod_fwd(d, t).wait_send()
        for c in range(n_chunk):
            swap(d, c).wait_send()
    halo_drain()
    for j in range(n_o):
        for k in range(4 if j else 5):
            if j == 0 and k == 0:
                continue
            for e in range(1, tp):
                share(e, j, k, t).wait_send()
        for a in range(2):
            side(j, a, i).wait_send()
            if j == 0:
                diag(0, a, nbr[a]).wait_send()
    for j in range(n_o):
        line_drain(held(j))
        if j > 0:
            cross(j, o).wait_send()
    for c in range(n_chunk):
        leave(c).wait()


def layer(sp, tp, vmem, cond, cctx, gain, table, *big):
    w_shift, latent, context, w_query = big[0], big[3], big[4], big[5]
    rows, width = latent.shape
    row_part, mod_cols = w_shift.shape
    cols = w_query.shape[1]
    heads = cols // HEAD_DIM
    tokens = rows * tp
    n_lat = 2 * tokens
    n_ctx = context.shape[0] * sp
    n_o = sp // INNER
    n_chunk = 2
    pack = -(-VECS * (mod_cols // LANES) // 8) * 8
    dma = pltpu.SemaphoreType.DMA
    spec = pl.BlockSpec(memory_space=pltpu.HBM)
    bf, f32 = jnp.bfloat16, jnp.float32
    pieces = rows // GRID_W
    step_rows = max(tokens, n_ctx // INNER + context.shape[0])
    return pl.pallas_call(
        functools.partial(layer_kernel, sp, tp),
        out_shape=jax.ShapeDtypeStruct(latent.shape, bf),
        in_specs=[spec] * 13,
        out_specs=spec,
        scratch_shapes=[
            VMEM(cond.shape, f32), VMEM(cctx.shape, f32), VMEM(gain.shape, f32),
            VMEM(table.shape, f32), VMEM(latent.shape, bf), dma((n_chunk,)),
            VMEM((row_part, mod_cols), bf), VMEM((row_part, mod_cols), bf),
            VMEM((row_part, mod_cols), bf),
            VMEM((tp, pack, LANES), f32),
            VMEM((n_lat, width), bf),
            VMEM((n_ctx, width), bf),
            VMEM((width, cols), bf), VMEM((width, cols), bf), VMEM((width, cols), bf),
            VMEM((cols, width), bf),
            VMEM((8, width), f32), VMEM((1, width), f32),
            VMEM((step_rows, width), bf), VMEM((step_rows, width), bf),
            VMEM((tokens, cols), bf),
            VMEM((n_lat + n_ctx, cols), bf), VMEM((n_lat + n_ctx, 2 * cols), bf),
            VMEM((heads, tokens, n_lat), f32),
            VMEM((tokens, cols), bf),
            VMEM((tokens, width), bf), VMEM((tp, rows, width), bf),
            dma((9,)), dma((4,)), dma((tp, n_chunk)), dma((tp, n_chunk)),
            VMEM((INNER, pack, LANES), f32),
            VMEM((n_o, pack, LANES), f32),
            dma((INNER,)), dma((INNER,)), dma((n_o,)), dma((n_o,)), dma((tp,)), dma((tp,)),
            dma((tp,)), dma((tp,)), dma((pieces,)), dma((pieces,)),
            dma((tp, pieces)), dma((tp, pieces)),
            dma((n_o, 2)), dma((n_o,)), dma((n_o,)), dma((n_o,)),
            dma((n_o, 2)), dma((n_o, 2)), dma((1, 2)), dma((1, 2)), dma((tp, n_o, 5)), dma((tp, n_o, 5)),
        ],
        compiler_params=pltpu.CompilerParams(
            collective_id=0, has_side_effects=True, vmem_limit_bytes=vmem
        ),
        name="layer",
    )(cond, cctx, gain, table, *big)


def on_device(
    latent, context, condition, ctx_cond, norm_gain, w_shift, w_scale, w_gate,
    w_query, w_key, w_value, w_out, rel_bias,
):
    tp = lax.axis_size("tp")
    sp = lax.axis_size("sp")
    tokens = latent.shape[0] * tp
    halo = HALF * GRID_W
    assert tokens == 2 * halo and tp % 2 == 0 and sp % (4 * INNER) == 0
    return layer(
        sp, tp, 55 * 1024 * 1024, condition[None], ctx_cond[None], norm_gain[None],
        jnp.transpose(rel_bias, (1, 0, 2)),
        w_shift, w_scale, w_gate, latent, context, w_query, w_key, w_value, w_out,
    )


def solution(mesh):
    placed = (
        P(("sp", "tp"), None),
        P("sp", None),
        P(),
        P(),
        P(),
        P("sp", "tp"),
        P("sp", "tp"),
        P("sp", "tp"),
        P(None, "tp"),
        P(None, "tp"),
        P(None, "tp"),
        P("tp", None),
        P(),
    )
    return jax.shard_map(
        on_device, mesh=mesh, in_specs=placed, out_specs=P(("sp", "tp"), None), check_vma=False
    )
```
